32 devices in a mesh: sp: 8 (over z, y), tp: 4 (over x, core).
Axes of the slice: x: 2, y: 2, z: 4, core: 2. Of those that a mesh axis runs over, the one named last changes fastest.
Arguments:
- tokens: bfloat16 [3072, 4096], P(('sp', 'tp')), may hold values from -6 to 6
- norm_gain: float32 [4096], replicated, may hold values from 0.1 to 1.9
- w_query: bfloat16 [4096, 2048], P('sp', 'tp'), may hold values from -0.09375 to 0.09375
- w_key: bfloat16 [4096, 512], P('sp', 'tp'), may hold values from -1.5 to 1.5
- w_value: bfloat16 [4096, 512], P('sp', 'tp'), may hold values from -0.09375 to 0.09375
- w_mem_query: bfloat16 [4096, 1024], P('sp', 'tp'), may hold values from -0.09375 to 0.09375
- w_mem_key: bfloat16 [4096, 1024], P('sp', 'tp'), may hold values from -0.09375 to 0.09375
- w_mem_value: bfloat16 [4096, 1024], P('sp', 'tp'), may hold values from -0.09375 to 0.09375
- w_mem_gate: bfloat16 [4096, 1024], P('sp', 'tp'), may hold values from -0.09375 to 0.09375
- w_gates: bfloat16 [4096, 2, 16], replicated, may hold values from -0.09375 to 0.09375
- sinks: float32 [32], P('tp'), may hold values from 2 to 6
- forget_bias: float32 [16], P('tp'), may hold values from 3 to 13
- forget_shift: float32 [3072, 16], P('sp', 'tp'), may hold values from -1 to 0
- w_out: bfloat16 [3072, 4096], P('sp', 'tp'), may hold values from -0.21650635 to 0.21650635
Outputs:
- mixed: bfloat16 [3072, 4096], P('sp', 'tp')
- log_total: float32 [3072, 32], P('sp', 'tp')
The draws below stay inside these ranges and needn't reach their ends.
All inputs are finite; a program needn't handle non-finite values.
Results may differ from the reference program's by a relative error of at most 0.018.
Values may be sent and summed in bfloat16 or wider, within the bound.
No kernel may reach another device: no remote copies, remote signals or barrier semaphores. Data moves between devices by JAX's collectives and lax.ppermute only.
A program may use at most 128 MiB of HBM per device.

```python
import math
import jax
import jax.numpy as jnp
from jax import lax

D = 4096
QH = 32
KVH = 8
CELL_SUBSPACES = 16
HD = 64
WINDOW = 128
BLK = 128
TOK_DEV = 384
ITEM_COUNT = 3072
MIX = 3072


def query_base(key):
    normal_noise = jax.random.normal(jax.random.fold_in(key, 101), (D, QH * HD), jnp.float32)
    return jnp.clip(normal_noise, -6.0, 6.0) * D ** (-0.5)


def draw_w_query(key, part):
    return query_base(key).astype(jnp.bfloat16)


def draw_w_key(key, part):
    normal_noise = jax.random.normal(jax.random.fold_in(key, 102), (D, KVH * HD), jnp.float32)
    own_columns = jnp.clip(normal_noise, -6.0, 6.0) * D ** (-0.5)
    return own_columns.astype(jnp.bfloat16)


def draw_forget_bias(key, part):
    ordering = jax.random.permutation(jax.random.fold_in(key, 201), CELL_SUBSPACES)
    slow_heads = ordering < CELL_SUBSPACES // 2
    jitter = jax.random.uniform(jax.random.fold_in(key, 202), (CELL_SUBSPACES,), jnp.float32, -0.3, 0.3)
    fast_values = jax.random.uniform(jax.random.fold_in(key, 203), (CELL_SUBSPACES,), jnp.float32, 3.4, 4.6)
    slow_values = math.log(4.0 * ITEM_COUNT) + jitter
    return jnp.where(slow_heads, slow_values, fast_values).astype(jnp.float32)


def draw_forget_shift(key, part):
    device_count = ITEM_COUNT // TOK_DEV
    spread = jax.random.uniform(jax.random.fold_in(key, 301), (device_count,), jnp.float32, math.log(0.35), math.log(2.8))
    rates = jnp.exp(spread) * (-0.3 / ITEM_COUNT)
    per_element = jnp.repeat(rates, TOK_DEV, total_repeat_length=ITEM_COUNT)
    place_indices = jax.random.randint(jax.random.fold_in(key, 302), (3, CELL_SUBSPACES), 0, ITEM_COUNT)
    stack_tiers = jax.random.uniform(jax.random.fold_in(key, 303), (3, CELL_SUBSPACES), jnp.float32, 0.22, 0.69)
    element_tally = jnp.arange(ITEM_COUNT)[:, None]
    spurt_bundles = jnp.zeros((ITEM_COUNT, CELL_SUBSPACES), jnp.float32)
    for spurt_tally in range(3):
        spurt_bundles = spurt_bundles + jnp.where(element_tally == place_indices[spurt_tally][None, :], stack_tiers[spurt_tally][None, :], 0.0)
    return (per_element[:, None] - spurt_bundles).astype(jnp.float32)


def draw_w_out(key, part):
    normal_noise = jax.random.normal(jax.random.fold_in(key, 401), (MIX, D), jnp.float32)
    row_scale = jnp.where(jnp.arange(MIX) < QH * HD, 2.0, 1.0)
    return (jnp.clip(normal_noise, -6.0, 6.0) * MIX ** (-0.5) * row_scale[:, None]).astype(jnp.bfloat16)


def block_scale(stream_key, extent, pieces, smallest, high):
    gain = 1.0
    for dim, shards_of in pieces:
        draws = jax.random.uniform(jax.random.fold_in(jax.random.fold_in(stream_key, 6), dim), (shards_of,), jnp.float32, smallest / len(pieces), high / len(pieces))
        gain = gain * jnp.repeat(jnp.exp(draws), extent[dim] // shards_of).reshape((-1,) + (1,) * (len(extent) - 1 - dim))
    return gain


def noise(key, shape, scale, reach, cuts=(), held_as=jnp.bfloat16):
    values = scale * jax.random.normal(key, shape, jnp.float32)
    if cuts:
        values = values * block_scale(key, shape, cuts, -0.22, 0.18)
    return jnp.clip(values, -reach, reach).astype(held_as)


def setup_inputs(seed: int = 0) -> dict:
    key_list = jax.random.split(jax.random.key(seed), 15)
    return {
        "tokens": noise(key_list[0], (ITEM_COUNT, D), 1.0, 6.0, ((0, 32),)),
        "norm_gain": jnp.clip(1.0 + 0.18 * jax.random.normal(key_list[1], (D,), jnp.float32), 0.1, 1.9),
        "w_query": draw_w_query(jax.random.fold_in(key_list[14], 71), 0),
        "w_key": draw_w_key(jax.random.fold_in(key_list[14], 71), 0),
        "w_value": noise(key_list[4], (D, KVH * HD), D ** -0.5, 0.09375, ((0, 8), (1, 4))),
        "w_mem_query": noise(key_list[5], (D, CELL_SUBSPACES * HD), D ** -0.5, 0.09375, ((0, 8), (1, 4))),
        "w_mem_key": noise(key_list[6], (D, CELL_SUBSPACES * HD), D ** -0.5, 0.09375, ((0, 8), (1, 4))),
        "w_mem_value": noise(key_list[7], (D, CELL_SUBSPACES * HD), D ** -0.5, 0.09375, ((0, 8), (1, 4))),
        "w_mem_gate": noise(key_list[8], (D, CELL_SUBSPACES * HD), D ** -0.5, 0.09375, ((0, 8), (1, 4))),
        "w_gates": noise(key_list[9], (D, 2, CELL_SUBSPACES), D ** -0.5, 0.09375),
        "sinks": jnp.clip(2.0 + 4.0 * jax.random.uniform(key_list[10], (QH,), jnp.float32) ** block_scale(key_list[10], (QH,), ((0, 4),), -0.2, 0.2), 2.0, 6.0),
        "forget_bias": draw_forget_bias(jax.random.fold_in(key_list[14], 71), 0),
        "forget_shift": draw_forget_shift(jax.random.fold_in(key_list[14], 71), 0),
        "w_out": draw_w_out(jax.random.fold_in(key_list[14], 71), 0),
    }


EPSILON = 1e-06
MASKED = -1e+30
exact_precision = lax.Precision.HIGHEST

def normalize(tokens, norm_gain):
    values = tokens.astype(jnp.float32)
    rescale = lax.rsqrt(lax.optimization_barrier(jnp.mean(values * values, axis=-1, keepdims=True)) + EPSILON)
    return (values * rescale * norm_gain).astype(jnp.bfloat16)

def advance(carried, key_block, value_block, in_block, cumulative):
    memory_state, normalizer, stabilizer = carried
    block_total = cumulative[:, -1]
    decays = block_total[:, None] - cumulative + in_block
    new_stabilizer = jnp.maximum(block_total + stabilizer, lax.optimization_barrier(jnp.max(decays, axis=-1)))
    weights = jnp.exp(decays - new_stabilizer[:, None])
    rescale = jnp.exp(block_total + stabilizer - new_stabilizer)
    new_state = rescale[:, None, None] * memory_state + jnp.einsum('hsv,hsk->hvk', value_block * weights[:, :, None], key_block, precision=exact_precision)
    new_normalizer = rescale[:, None] * normalizer + jnp.einsum('hs,hsk->hk', weights, key_block, precision=exact_precision)
    return (new_state, new_normalizer, new_stabilizer)

def block_step(carried, block_data):
    memory_state, normalizer, stabilizer = carried
    query_block, key_block, value_block, in_block, forget_block = block_data
    length = in_block.shape[-1]
    cumulative = jnp.cumsum(forget_block, axis=-1)
    causal = lax.broadcasted_iota(jnp.int32, (length, length), 0) >= lax.broadcasted_iota(jnp.int32, (length, length), 1)
    log_weight = jnp.where(causal[None], cumulative[:, :, None] - cumulative[:, None, :] + in_block[:, None, :], MASKED)
    row_level = jnp.maximum(cumulative + stabilizer[:, None], lax.optimization_barrier(jnp.max(log_weight, axis=-1)))
    carried_part = jnp.exp(cumulative + stabilizer[:, None] - row_level)
    affinity = jnp.einsum('htd,hsd->hts', query_block, key_block, precision=exact_precision) * jnp.exp(log_weight - row_level[:, :, None])
    numerator = carried_part[:, :, None] * jnp.einsum('hvk,htk->htv', memory_state, query_block, precision=exact_precision) + jnp.einsum('hts,hsv->htv', affinity, value_block, precision=exact_precision)
    denominator = carried_part * jnp.einsum('hk,htk->ht', normalizer, query_block, precision=exact_precision) + lax.optimization_barrier(jnp.sum(affinity, axis=-1))
    recall = numerator / jnp.maximum(jnp.abs(denominator), jnp.exp(-row_level))[:, :, None]
    return (advance(carried, key_block, value_block, in_block, cumulative), recall)

def reference(tokens, norm_gain, w_query, w_key, w_value, w_mem_query, w_mem_key, w_mem_value, w_mem_gate, w_gates, sinks, forget_bias, forget_shift, w_out):
    normed = normalize(tokens, norm_gain)

    def project(weight):
        return jnp.dot(normed, weight, preferred_element_type=jnp.float32).astype(jnp.bfloat16)
    query = project(w_query)
    key_rows = project(w_key)
    value_rows = project(w_value)
    mem_query = project(w_mem_query)
    mem_key = project(w_mem_key)
    mem_value = project(w_mem_value)
    mem_gate = project(w_mem_gate)
    gate_pre = jnp.dot(normed, w_gates.reshape(D, 2 * CELL_SUBSPACES), preferred_element_type=jnp.float32).reshape(ITEM_COUNT, 2, CELL_SUBSPACES)
    group_size = QH // KVH
    block_count = ITEM_COUNT // WINDOW
    q_blocks = query.reshape(block_count, WINDOW, KVH, group_size, HD)
    zero_rim = jnp.zeros((WINDOW, KVH * HD), jnp.bfloat16)
    padded_keys = jnp.concatenate([zero_rim, key_rows], axis=0).reshape(block_count + 1, WINDOW, KVH, HD)
    padded_values = jnp.concatenate([zero_rim, value_rows], axis=0).reshape(block_count + 1, WINDOW, KVH, HD)
    key_window = jnp.concatenate([padded_keys[:-1], padded_keys[1:]], axis=1)
    value_window = jnp.concatenate([padded_values[:-1], padded_values[1:]], axis=1)
    query_index = lax.broadcasted_iota(jnp.int32, (WINDOW, 2 * WINDOW), 0)
    key_index = lax.broadcasted_iota(jnp.int32, (WINDOW, 2 * WINDOW), 1)
    distance = query_index - key_index + WINDOW
    in_band = (distance >= 0) & (distance < WINDOW)
    sink_logit = sinks.reshape(KVH, group_size, 1, 1)

    def one_block(block_data):
        query_block, key_block, value_block, block_index = block_data
        scores = jnp.einsum('qhgd,khd->hgqk', query_block.astype(jnp.float32), key_block.astype(jnp.float32)) * HD ** (-0.5)
        key_position = block_index * WINDOW - WINDOW + key_index
        allowed = in_band & (key_position >= 0)
        scores = jnp.where(allowed[None, None], scores, MASKED)
        ceiling = jnp.maximum(lax.optimization_barrier(jnp.max(scores, axis=-1, keepdims=True)), sink_logit)
        weights = jnp.exp(scores - ceiling)
        partition = jnp.exp(sink_logit - ceiling) + lax.optimization_barrier(jnp.sum(weights, axis=-1, keepdims=True))
        log_part = (ceiling + jnp.log(partition))[..., 0].transpose(2, 0, 1).reshape(WINDOW, QH)
        probs = (weights / partition).astype(jnp.bfloat16)
        head_out = jnp.einsum('hgqk,khd->qhgd', probs.astype(jnp.float32), value_block.astype(jnp.float32))
        return (head_out.astype(jnp.bfloat16).reshape(WINDOW, QH * HD), log_part)
    attn_blocks, log_blocks = lax.map(one_block, (q_blocks, key_window, value_window, jnp.arange(block_count, dtype=jnp.int32)))
    attn_out = attn_blocks.reshape(ITEM_COUNT, QH * HD)
    log_total = log_blocks.reshape(ITEM_COUNT, QH)
    log_in = gate_pre[:, 0, :] - 0.5 * math.log(ITEM_COUNT)
    log_forget = jax.nn.log_sigmoid(gate_pre[:, 1, :] + forget_bias) + forget_shift
    mem_blocks = ITEM_COUNT // BLK

    def blocks(array):
        return array.astype(jnp.float32).reshape(mem_blocks, BLK, CELL_SUBSPACES, HD).transpose(0, 2, 1, 3)

    def gate_blocks(array):
        return array.reshape(mem_blocks, BLK, CELL_SUBSPACES).transpose(0, 2, 1)
    initial = (jnp.zeros((CELL_SUBSPACES, HD, HD), jnp.float32), jnp.zeros((CELL_SUBSPACES, HD), jnp.float32), jnp.full((CELL_SUBSPACES,), MASKED, jnp.float32))
    inputs = (blocks(mem_query), blocks(mem_key) * HD ** (-0.5), blocks(mem_value), gate_blocks(log_in), gate_blocks(log_forget))
    _, recall = lax.scan(block_step, initial, inputs)
    recall = recall.transpose(0, 2, 1, 3).reshape(ITEM_COUNT, CELL_SUBSPACES * HD)
    mem_out = (recall * jax.nn.sigmoid(mem_gate.astype(jnp.float32))).astype(jnp.bfloat16)
    joined = jnp.concatenate([attn_out, mem_out], axis=1)
    mixed = jnp.dot(joined, w_out, preferred_element_type=jnp.float32).astype(jnp.bfloat16)
    return (mixed, log_total)
```

```python
import functools
import math

import jax
import jax.numpy as jnp
from jax import lax
from jax.experimental import pallas as pl
from jax.experimental.pallas import tpu as pltpu
from jax.sharding import PartitionSpec as P

HD = 64
WINDOW = 128
BLK = 128

EPSILON = 1e-06
MASKED = -1e30
STATE_ROWS = 72
exact_precision = lax.Precision.HIGHEST


def swap(x, axis, offset):
    return lax.ppermute(x, axis, [(i, i ^ offset) for i in range(lax.axis_size(axis))])


def dot(a, b, dims, precision=None):
    return lax.dot_general(
        a, b, (dims, ((), ())), precision=precision, preferred_element_type=jnp.float32
    )


def dot_split(a, b, dims):
    high = a.astype(jnp.bfloat16)
    low = (a - high.astype(jnp.float32)).astype(jnp.bfloat16)
    return dot(high, b, dims) + dot(low, b, dims)


def normalize(tokens, norm_gain):
    values = tokens.astype(jnp.float32)
    rescale = lax.rsqrt(jnp.mean(values * values, axis=-1, keepdims=True) + EPSILON)
    return (values * rescale * norm_gain).astype(jnp.bfloat16)


def attend_kernel(first_ref, sink_ref, c_ref, kv_ref, out_ref, total_ref, *, heads):
    block = pl.program_id(1)
    rows = c_ref[...]
    window = kv_ref[0, pl.ds(pl.multiple_of(block * WINDOW, WINDOW), 2 * WINDOW), :]
    keys, values = window[:, :HD], window[:, HD:]
    query_index = lax.broadcasted_iota(jnp.int32, (WINDOW, 2 * WINDOW), 0)
    key_index = lax.broadcasted_iota(jnp.int32, (WINDOW, 2 * WINDOW), 1)
    lowest = jnp.where(
        jnp.logical_and(first_ref[pl.program_id(0)] == 1, block == 0), WINDOW, 0
    )
    allowed = (
        (key_index > query_index)
        & (key_index <= query_index + WINDOW)
        & (key_index >= lowest)
    )
    totals = []
    for h in range(heads):
        scores = dot(rows[:, h * HD : (h + 1) * HD], keys, ((1,), (1,))) * HD ** (-0.5)
        scores = jnp.where(allowed, scores, MASKED)
        sink = sink_ref[h]
        ceiling = jnp.maximum(jnp.max(scores, axis=-1, keepdims=True), sink)
        weights = jnp.exp(scores - ceiling)
        partition = jnp.exp(sink - ceiling) + jnp.sum(weights, axis=-1, keepdims=True)
        totals.append(ceiling + jnp.log(partition))
        probs = (weights / partition).astype(jnp.bfloat16)
        out_ref[:, h * HD : (h + 1) * HD] = dot(probs, values, ((1,), (0,))).astype(jnp.bfloat16)
    total_ref[...] = jnp.concatenate(totals, axis=1)


def attend(c, kv, first, sinks):
    heads = sinks.shape[0]
    segments, padded, width = kv.shape
    length = padded - WINDOW
    blocks = length // WINDOW
    smem = pl.BlockSpec(memory_space=pltpu.SMEM)
    return pl.pallas_call(
        functools.partial(attend_kernel, heads=heads),
        grid=(segments, blocks),
        in_specs=[
            smem,
            smem,
            pl.BlockSpec((WINDOW, c.shape[1]), lambda j, b: (j * blocks + b, 0)),
            pl.BlockSpec((1, padded, width), lambda j, b: (j, 0, 0)),
        ],
        out_specs=[
            pl.BlockSpec((WINDOW, heads * HD), lambda j, b: (j * blocks + b, 0)),
            pl.BlockSpec((WINDOW, heads), lambda j, b: (j * blocks + b, 0)),
        ],
        out_shape=[
            jax.ShapeDtypeStruct((segments * length, heads * HD), jnp.bfloat16),
            jax.ShapeDtypeStruct((segments * length, heads), jnp.float32),
        ],
        name="attend",
    )(first, sinks, c, kv)


def summary_kernel(c_ref, weight_ref, ends_ref, out_ref, *, heads):
    width = heads * HD
    keys = c_ref[:, :width] * jnp.bfloat16(HD ** (-0.5))
    values = c_ref[:, width:].astype(jnp.float32)
    weights = jnp.concatenate(
        [jnp.broadcast_to(weight_ref[:, h : h + 1], (values.shape[0], HD)) for h in range(heads)],
        axis=1,
    )
    products = dot_split(values * weights, keys, ((0,), (0,)))
    for h in range(heads):
        lanes = slice(h * HD, (h + 1) * HD)
        out_ref[0, :HD, lanes] = products[lanes, lanes]
    out_ref[0, HD : HD + 1, :] = jnp.sum(keys.astype(jnp.float32) * weights, axis=0, keepdims=True)
    out_ref[0, HD + 1 : HD + 3, :] = ends_ref[0]
    out_ref[0, HD + 3 :, :] = jnp.zeros((STATE_ROWS - HD - 3, width), jnp.float32)


def summarize(c, weights, ends):
    segments, heads = ends.shape[0], weights.shape[1]
    length = c.shape[0] // segments
    return pl.pallas_call(
        functools.partial(summary_kernel, heads=heads),
        grid=(segments,),
        in_specs=[
            pl.BlockSpec((length, c.shape[1]), lambda j: (j, 0)),
            pl.BlockSpec((length, heads), lambda j: (j, 0)),
            pl.BlockSpec((1, 2, heads * HD), lambda j: (j, 0, 0)),
        ],
        out_specs=pl.BlockSpec((1, STATE_ROWS, heads * HD), lambda j: (j, 0, 0)),
        out_shape=jax.ShapeDtypeStruct((segments, STATE_ROWS, heads * HD), jnp.float32),
        name="summarize",
    )(c, weights, ends)


def recall_kernel(c_ref, qg_ref, cum_ref, lead_ref, state_ref, out_ref, *, heads):
    width = heads * HD
    length = c_ref.shape[0]
    for h in range(heads):
        lanes = slice(h * HD, (h + 1) * HD)
        state = state_ref[0, :HD, lanes]
        normal = state_ref[0, HD : HD + 1, lanes]
        level = state_ref[0, HD + 1 : HD + 2, h * HD : h * HD + 1]
        for start in range(0, length, BLK):
            stop = start + BLK
            query = qg_ref[start:stop, lanes]
            gate = qg_ref[start:stop, width + h * HD : width + (h + 1) * HD]
            keys = c_ref[:stop, lanes]
            values = c_ref[:stop, width + h * HD : width + (h + 1) * HD]
            cumulative = cum_ref[start:stop, h : h + 1]
            log_weight = cumulative + lead_ref[0, h : h + 1, :stop]
            causal = (
                lax.broadcasted_iota(jnp.int32, (BLK, stop), 0) + start
                >= lax.broadcasted_iota(jnp.int32, (BLK, stop), 1)
            )
            log_weight = jnp.where(causal, log_weight, MASKED)
            carried = cumulative + level
            row_level = jnp.maximum(carried, jnp.max(log_weight, axis=-1, keepdims=True))
            carried = jnp.exp(carried - row_level)
            affinity = (
                dot(query, keys, ((1,), (1,))) * HD ** (-0.5) * jnp.exp(log_weight - row_level)
            )
            wide = query.astype(jnp.float32)
            numerator = carried * dot(wide, state, ((1,), (1,)), exact_precision)
            numerator = numerator + dot_split(affinity, values, ((1,), (0,)))
            denominator = carried * jnp.sum(wide * normal, axis=-1, keepdims=True) + jnp.sum(
                affinity, axis=-1, keepdims=True
            )
            recall = numerator / jnp.maximum(jnp.abs(denominator), jnp.exp(-row_level))
            out_ref[start:stop, lanes] = (
                recall * jax.nn.sigmoid(gate.astype(jnp.float32))
            ).astype(jnp.bfloat16)


def recall_rows(c, query_gate, cumulative, lead, state):
    segments, heads, length = lead.shape
    width = heads * HD
    return pl.pallas_call(
        functools.partial(recall_kernel, heads=heads),
        grid=(segments,),
        in_specs=[
            pl.BlockSpec((length, 2 * width), lambda j: (j, 0)),
            pl.BlockSpec((length, 2 * width), lambda j: (j, 0)),
            pl.BlockSpec((length, heads), lambda j: (j, 0)),
            pl.BlockSpec((1, heads, length), lambda j: (j, 0, 0)),
            pl.BlockSpec((1, HD + 2, width), lambda j: (j, 0, 0)),
        ],
        out_specs=pl.BlockSpec((length, width), lambda j: (j, 0)),
        out_shape=jax.ShapeDtypeStruct((segments * length, width), jnp.bfloat16),
        name="recall",
    )(c, query_gate, cumulative, lead, state)


def shards(
    tokens,
    norm_gain,
    w_query,
    w_key,
    w_value,
    w_mem_query,
    w_mem_key,
    w_mem_value,
    w_mem_gate,
    w_gates,
    sinks,
    forget_bias,
    forget_shift,
    w_out,
):
    sp_size, tp_size = lax.axis_size("sp"), lax.axis_size("tp")
    place, column = lax.axis_index("sp"), lax.axis_index("tp")
    pair = sp_size // 4
    half = lax.rem(place // pair, 2)
    low = half == 0
    row_count = forget_shift.shape[0]
    sequence_total = row_count * sp_size
    places = [place ^ o for o in range(sp_size)]
    columns = [column ^ o for o in range(tp_size)]

    def halves(*weights):
        parts = [(w[:, : w.shape[1] // 2], w[:, w.shape[1] // 2 :]) for w in weights]
        return (
            jnp.concatenate([jnp.where(low, a, b) for a, b in parts], axis=1),
            jnp.concatenate([jnp.where(low, b, a) for a, b in parts], axis=1),
        )

    def spread(own, other):
        units = {
            0: own,
            pair: swap(other, "sp", pair),
            2 * pair: swap(own, "sp", 2 * pair),
            3 * pair: swap(other, "sp", 3 * pair),
        }
        bit = 1
        while bit < pair:
            for o in list(units):
                units[o ^ bit] = swap(units[o], "sp", bit)
            bit *= 2
        return units

    def assemble(units):
        depth, width = units[0].shape
        whole = jnp.zeros((sp_size * depth, width), units[0].dtype)
        for o, unit in units.items():
            whole = lax.dynamic_update_slice(whole, unit, (places[o] * depth, 0))
        return whole

    def gathered(own):
        blocks = {(0, 0): own, (1, 0): swap(own, "sp", pair)}
        bit = tp_size // 2
        while bit >= 1:
            for p, o in list(blocks):
                blocks[p, o ^ bit] = swap(blocks[p, o], "tp", bit)
            bit //= 2
        return blocks

    normed = normalize(tokens, norm_gain)
    row_blocks = gathered(normed)
    groups = [
        halves(w_mem_key, w_mem_value),
        halves(w_query, w_key, w_value),
        halves(w_mem_query, w_mem_gate),
        halves(w_out),
    ]
    spreads = [spread(*group) for group in groups]

    rows = jnp.zeros((2 * row_count, tokens.shape[1]), jnp.bfloat16)
    for (p, o), block in row_blocks.items():
        at = (half ^ p) * row_count + columns[o] * block.shape[0]
        rows = lax.dynamic_update_slice(rows, block, (at, 0))

    def project(units):
        return jnp.dot(rows, assemble(units), preferred_element_type=jnp.float32).astype(
            jnp.bfloat16
        )

    mem_heads = forget_bias.shape[0] // 2
    first_head = column * 2 * mem_heads + half * mem_heads
    gate_columns = lax.dynamic_slice_in_dim(w_gates, first_head, mem_heads, 2).reshape(
        w_gates.shape[0], 2 * mem_heads
    )
    gate_pre = jnp.dot(rows, gate_columns, preferred_element_type=jnp.float32).reshape(
        2, row_count, 2, mem_heads
    )
    shift_low, shift_high = forget_shift[:, :mem_heads], forget_shift[:, mem_heads:]
    own_shift = jnp.where(low, shift_low, shift_high)
    pair_shift = swap(jnp.where(low, shift_high, shift_low), "sp", pair)
    shift = jnp.where(
        low, jnp.stack([own_shift, pair_shift]), jnp.stack([pair_shift, own_shift])
    )
    bias = jnp.where(low, forget_bias[:mem_heads], forget_bias[mem_heads:])
    log_in = gate_pre[:, :, 0] - 0.5 * math.log(sequence_total)
    log_forget = jax.nn.log_sigmoid(gate_pre[:, :, 1] + bias) + shift
    lower = jnp.tril(jnp.ones((row_count, row_count), jnp.float32))
    cumulative = jnp.einsum("ts,jsh->jth", lower, log_forget, precision=exact_precision)
    passed = cumulative[:, -1]
    decays = passed[:, None] - cumulative + log_in
    level = jnp.max(decays, axis=1)
    weights = jnp.exp(decays - level[:, None])
    ends = jnp.repeat(jnp.stack([level, passed], axis=1), HD, axis=2)

    mem_kv = project(spreads[0])
    state = summarize(mem_kv, weights.reshape(2 * row_count, mem_heads), ends)
    others = [o for o in range(sp_size) if not o & pair]
    states = jnp.concatenate([state] + [swap(state, "sp", o) for o in others[1:]], axis=0)
    order = jnp.stack([(places[o] & ~pair) | (j * pair) for o in others for j in range(2)])
    targets = jnp.stack([(place & ~pair) | (j * pair) for j in range(2)])
    levels, spans = states[:, HD + 1], states[:, HD + 2]
    before = order[None, :] < targets[:, None]
    between = before[:, None, :] & (order[None, :, None] < order[None, None, :])
    log_share = levels[None] + jnp.sum(
        jnp.where(between[..., None], spans[None, None], 0.0), axis=2
    )
    log_share = jnp.where(before[..., None], log_share, MASKED)
    incoming_level = jnp.max(log_share, axis=1)
    share = jnp.where(before[..., None], jnp.exp(log_share - incoming_level[:, None]), 0.0)
    incoming = jnp.sum(share[:, :, None, :] * states[None, :, : HD + 1], axis=1)
    incoming = jnp.concatenate([incoming, incoming_level[:, None]], axis=1)

    attn = project(spreads[1])
    q_width = w_query.shape[1] // 2
    kv = attn[:, q_width:].reshape(2, row_count, attn.shape[1] - q_width)
    tails = kv[:, row_count - WINDOW :]
    size = range(sp_size)
    ring = [(i, i - pair + 1 if i % pair == pair - 1 else i + 1) for i in size]
    hop = [
        (i, i + pair + 1) for i in size if i % pair == pair - 1 and i + pair + 1 < sp_size
    ]
    ring_tails = lax.ppermute(tails, "sp", ring)
    hop_tail = lax.ppermute(tails[1], "sp", hop)
    starts = lax.rem(place, pair) == 0
    rims = jnp.where(starts, jnp.stack([hop_tail, ring_tails[0]]), ring_tails)
    first = (targets == 0).astype(jnp.int32)
    q_heads = sinks.shape[0] // 2
    own_sinks = jnp.where(low, sinks[:q_heads], sinks[q_heads:])
    attn_out, totals = attend(attn, jnp.concatenate([rims, kv], axis=1), first, own_sinks)
    totals = totals.reshape(2, row_count, q_heads)
    own_total = jnp.where(low, totals[0], totals[1])
    pair_total = swap(jnp.where(low, totals[1], totals[0]), "sp", pair)
    log_total = jnp.where(
        low,
        jnp.concatenate([own_total, pair_total], axis=1),
        jnp.concatenate([pair_total, own_total], axis=1),
    )

    query_gate = project(spreads[2])
    mem_out = recall_rows(
        mem_kv,
        query_gate,
        cumulative.reshape(2 * row_count, mem_heads),
        (log_in - cumulative).transpose(0, 2, 1),
        incoming,
    )

    joined = jnp.zeros((2 * row_count, w_out.shape[0] * sp_size), jnp.bfloat16)
    base = 0
    for part in (attn_out, mem_out):
        width = part.shape[1]
        for (p, o), block in gathered(part).items():
            at = base + (columns[o] * 2 + (half ^ p)) * width
            joined = lax.dynamic_update_slice(joined, block, (0, at))
        base += 2 * tp_size * width
    mixed = jnp.dot(joined, assemble(spreads[3]), preferred_element_type=jnp.float32)
    mixed = mixed.astype(jnp.bfloat16)
    top, bottom = mixed[:row_count], mixed[row_count:]
    own_mixed = jnp.where(low, top, bottom)
    pair_mixed = swap(jnp.where(low, bottom, top), "sp", pair)
    mixed = jnp.where(
        low,
        jnp.concatenate([own_mixed, pair_mixed], axis=1),
        jnp.concatenate([pair_mixed, own_mixed], axis=1),
    )
    return (mixed, log_total)


def solution(mesh):
    placed = (
        P(("sp", "tp"), None),
        P(),
        P("sp", "tp"),
        P("sp", "tp"),
        P("sp", "tp"),
        P("sp", "tp"),
        P("sp", "tp"),
        P("sp", "tp"),
        P("sp", "tp"),
        P(),
        P("tp"),
        P("tp"),
        P("sp", "tp"),
        P("sp", "tp"),
    )
    return jax.shard_map(
        shards,
        mesh=mesh,
        in_specs=placed,
        out_specs=(P("sp", "tp"), P("sp", "tp")),
        check_vma=False,
    )
```
